32 devices in a mesh: fs: 8 (over z, y), tp: 4 (over x, core).
Axes of the slice: x: 2, y: 2, z: 4, core: 2. Of those that a mesh axis runs over, the one named last changes fastest.
Arguments:
- inputs: bfloat16 [4608, 2048], P('fs'), may hold values from -6 to 6
- query_cotangent: bfloat16 [4608, 1024], P('fs', 'tp'), may hold values from -0.017944336 to 0.017944336
- value_cotangent: bfloat16 [4608, 1024], P('fs', 'tp'), may hold values from -0.017944336 to 0.017944336
- weights_query: float32 [2048, 1024], P('fs', 'tp'), may hold values from -6 to 6
- weights_value: float32 [2048, 1024], P('fs', 'tp'), may hold values from -6 to 6
- basis_query: bfloat16 [1024, 32], P('tp'), may hold values from -0.75 to 0.75
- basis_value: bfloat16 [1024, 32], P('tp'), may hold values from -0.75 to 0.75
- first_query: float32 [2048, 512], P('fs', 'tp'), may hold values from -5.4 to 5.4, as said below
- second_query: float32 [2048, 512], P('fs', 'tp'), may hold values from 0.05 to 1
- first_value: float32 [2048, 512], P('fs', 'tp'), may hold values from -5.4 to 5.4, as said below
- second_value: float32 [2048, 512], P('fs', 'tp'), may hold values from 0.05 to 1
Outputs:
- step_query: float32 [2048, 1024], P('fs', 'tp')
- step_value: float32 [2048, 1024], P('fs', 'tp')
- new_query: float32 [2048, 1024], P('fs', 'tp')
- new_value: float32 [2048, 1024], P('fs', 'tp')
- copy_query: bfloat16 [2048, 1024], P(None, 'tp')
- copy_value: bfloat16 [2048, 1024], P(None, 'tp')
- moment_query: float32 [2048, 512], P('fs', 'tp')
- square_query: float32 [2048, 512], P('fs', 'tp')
- moment_value: float32 [2048, 512], P('fs', 'tp')
- square_value: float32 [2048, 512], P('fs', 'tp')
The draws below stay inside these ranges and needn't reach their ends.
Inputs may be any that keep to these rules, and one draw needn't show every extreme that they name: `first_query`: first moments, with a spread of scale from row to row. `first_value`: first moments, with a spread of scale from row to row.
All inputs are finite; a program needn't handle non-finite values.
Results may differ from the reference program's by a relative error of at most 0.003.
Values may be sent and summed in bfloat16 or wider, within the bound.
A program may use at most 64 MiB of HBM per device.

```python
import math
import jax
import jax.numpy as jnp
from jax import lax

D = 2048
HEADS = 16
HEAD = 64
RK = 32
FW = 1024
TOKENS = 4608


def moment_draw(key):
    base = 0.3 * jnp.clip(jax.random.normal(jax.random.fold_in(key, 11), (D, HEADS * RK), jnp.float32), -4.0, 4.0)
    factor = jnp.exp(jax.random.uniform(jax.random.fold_in(key, 12), (D, 1), jnp.float32, -1.5, 1.5))
    return base * factor


def draw_first_query(key, part):
    return moment_draw(jax.random.fold_in(key, 1))


def draw_first_value(key, part):
    return moment_draw(jax.random.fold_in(key, 2))


def raised(drawn, own_key, source, target, parts, factor):
    owner, partner = [(jnp.arange(drawn.shape[position]) // (drawn.shape[position] // parts)).reshape([-1 if axis == position else 1 for axis in range(drawn.ndim)]) for position in (source, target)]
    chosen = jax.random.permutation(own_key, parts)[partner]
    strong = (owner == chosen) | (owner == (partner + parts // 2) % parts)
    return jnp.where(strong, factor * drawn, drawn)


def block_levels(rng, shape, cuts, smallest, high):
    level, own = 1.0, jax.random.fold_in(rng, 6)
    for axis_at, shards_of in cuts:
        heights = jnp.exp(jax.random.uniform(jax.random.fold_in(own, axis_at), (shards_of,), jnp.float32, smallest / len(cuts), high / len(cuts)))
        level = level * jnp.repeat(heights, shape[axis_at] // shards_of).reshape([-1 if axis == axis_at else 1 for axis in range(len(shape))])
    return level


def bell_draw(rng, dims, width, bound, cuts=(), held_as=jnp.bfloat16):
    entries = jax.random.normal(rng, dims, jnp.float32) * width
    if len(cuts) > 0:
        entries = block_levels(rng, dims, cuts, -0.22, 0.18) * entries
    return jnp.clip(entries, min=-bound, max=bound).astype(held_as)


def bell_draw_with(rng, extent, width, most, cuts, heavy, dtype=jnp.bfloat16):
    drawn = width * jax.random.normal(rng, extent, jnp.float32)
    if cuts:
        drawn = drawn * block_levels(rng, extent, cuts, -0.22, 0.18)
    return jnp.clip(raised(drawn, jax.random.fold_in(rng, 3), *heavy), -most, most).astype(dtype)


def setup_inputs(seed: int = 0) -> dict:
    key_list = jax.random.split(jax.random.key(seed), 12)
    inputs = bell_draw_with(key_list[0], (TOKENS, D), 1.0, 6.0, ((0, 8),), (0, 1, 8, 2.0))
    query_cotangent = bell_draw(key_list[1], (TOKENS, FW), 0.003, 0.017944336, ((0, 8), (1, 4)))
    value_cotangent = bell_draw(key_list[2], (TOKENS, FW), 0.003, 0.017944336, ((0, 8), (1, 4)))
    weights_query = bell_draw(key_list[3], (D, FW), 1.0, 6.0, ((0, 8), (1, 4)), jnp.float32)
    weights_value = bell_draw(key_list[4], (D, FW), 1.0, 6.0, ((0, 8), (1, 4)), jnp.float32)
    basis_query = bell_draw(key_list[5], (FW, RK), HEAD ** -0.5, 0.75, ((0, 4),))
    basis_value = bell_draw(key_list[6], (FW, RK), HEAD ** -0.5, 0.75, ((0, 4),))
    first_query = draw_first_query(jax.random.fold_in(key_list[11], 71), 0)
    second_query = jnp.clip(jnp.exp(math.log(1.0) - 2.9957323 * jax.random.uniform(key_list[8], (D, HEADS * RK), jnp.float32) ** block_levels(key_list[8], (D, HEADS * RK), ((0, 8), (1, 4)), -0.2, 0.2)), 0.05, 1.0)
    first_value = draw_first_value(jax.random.fold_in(key_list[11], 71), 0)
    second_value = jnp.clip(jnp.exp(math.log(1.0) - 2.9957323 * jax.random.uniform(key_list[10], (D, HEADS * RK), jnp.float32) ** block_levels(key_list[10], (D, HEADS * RK), ((0, 8), (1, 4)), -0.2, 0.2)), 0.05, 1.0)
    return {"inputs": inputs, "query_cotangent": query_cotangent, "value_cotangent": value_cotangent, "weights_query": weights_query, "weights_value": weights_value, "basis_query": basis_query, "basis_value": basis_value, "first_query": first_query, "second_query": second_query, "first_value": first_value, "second_value": second_value}


def apply_basis(gradient, basis):
    split = gradient.reshape(D, HEADS, HEAD)
    factor = basis.reshape(HEADS, HEAD, RK).astype(jnp.float32)
    out = jnp.einsum('nhd,hdr->nhr', split, factor, precision=lax.Precision.HIGHEST)
    return out.reshape(D, HEADS * RK)

def expand(direction, basis):
    split = direction.reshape(D, HEADS, RK)
    factor = basis.reshape(HEADS, HEAD, RK).astype(jnp.float32)
    out = jnp.einsum('nhr,hdr->nhd', split, factor, precision=lax.Precision.HIGHEST)
    return out.reshape(D, HEADS * HEAD)

def update(inputs, cotangent, weights, basis, first, second):
    gradient = jnp.dot(inputs.T, cotangent, preferred_element_type=jnp.float32)
    reduced = apply_basis(gradient, basis)
    moment = 0.9 * first + 0.1 * reduced
    square = 0.95 * second + 0.05 * reduced * reduced
    direction = moment / (jnp.sqrt(square) + 1e-08)
    scale = 1.0 / jnp.sqrt(jnp.mean(direction * direction) + 0.25)
    step = scale * expand(direction, basis)
    fresh = weights - 0.1 * step
    return (step, fresh, fresh.astype(jnp.bfloat16), moment, square)

def reference(inputs, query_cotangent, value_cotangent, weights_query, weights_value, basis_query, basis_value, first_query, second_query, first_value, second_value):
    step_q, new_q, copy_q, moment_q, square_q = update(inputs, query_cotangent, weights_query, basis_query, first_query, second_query)
    step_v, new_v, copy_v, moment_v, square_v = update(inputs, value_cotangent, weights_value, basis_value, first_value, second_value)
    return (step_q, step_v, new_q, new_v, copy_q, copy_v, moment_q, square_q, moment_v, square_v)
```

```python
import functools

import jax
import jax.numpy as jnp
from jax import lax
from jax.experimental import pallas as pl
from jax.experimental.pallas import tpu as pltpu
from jax.sharding import PartitionSpec as P

HEAD = 64
RK = 32
CUT = 2
MESH = pl.DeviceIdType.MESH
F32 = jnp.float32
BF16 = jnp.bfloat16


def flip(x, bits):
    out, weight = x, 1
    while weight <= bits:
        if bits & weight:
            out = out + weight * (1 - 2 * ((x // weight) % 2))
        weight *= 2
    return out


def remote(src, dst, send, recv, to):
    return pltpu.make_async_remote_copy(
        src_ref=src, dst_ref=dst, send_sem=send, recv_sem=recv, device_id=to, device_id_type=MESH
    )


def body(
    n,
    t,
    x_hbm,
    cq_hbm,
    cv_hbm,
    wq_hbm,
    wv_hbm,
    bq_hbm,
    bv_hbm,
    fq_hbm,
    sq_hbm,
    fv_hbm,
    sv_hbm,
    step,
    new,
    copy,
    mom,
    sqr,
    x,
    cot,
    w,
    basis,
    first,
    second,
    small,
    part,
    summed,
    arrived1,
    arrived2,
    raw,
    tot,
    tot_all,
    in_sem,
    x_sem,
    s1,
    r1,
    s2,
    r2,
    st,
    rt,
    so,
    sr,
    rz,
    sy,
    ry,
    sn,
    rn,
    rm,
):
    f = lax.axis_index("fs")
    g = lax.axis_index("tp")
    me = f * t + g
    count = n * t
    outer = n // 2
    a, b = f // 2, f % 2
    mate = (a * 2 + 1 - b, g)
    depth = x.shape[1]
    rows = depth // n
    cols = w.shape[2]
    wide = cols // HEAD * RK
    cut = rz.shape[2]
    bit = rows // cut

    chunk = max(2 * rows, min(depth, 256))
    chunks = depth // chunk
    pairs = chunk // (2 * rows)
    order = list(range(chunks // 2, chunks)) + list(range(chunks // 2 - 1, -1, -1))
    at = a // pairs

    def chunk_at(k):
        return pl.ds(pl.multiple_of(flip(at, order[k]) * chunk, chunk), chunk)

    sources = ((bq_hbm, bv_hbm), (cq_hbm, cv_hbm), (fq_hbm, fv_hbm), (sq_hbm, sv_hbm), (wq_hbm, wv_hbm))
    holders = (basis, cot, first, second, w)

    def load(i):
        for p in range(2):
            pltpu.make_async_copy(sources[i][p], holders[i].at[p], in_sem.at[i]).start()

    def loaded(i):
        pltpu.make_async_copy(holders[i], holders[i], in_sem.at[i]).wait()

    x_loads = [
        pltpu.make_async_copy(x_hbm.at[:, chunk_at(k)], x.at[:, chunk_at(k)], x_sem.at[k])
        for k in range(chunks)
    ]
    load(0)
    load(1)
    x_loads[0].start()

    barrier = pltpu.get_barrier_semaphore()

    def hello(to):
        pl.semaphore_signal(barrier, inc=1, device_id=to, device_id_type=MESH)

    def greet_line(i, c):
        hello(((a + 1 + i) % outer * 2 + b, g))
        return c

    hello(mate)
    lax.fori_loop(0, outer - 1, greet_line, 0)
    for i in range(1, t):
        hello((f, (g + i) % t))
    for x_load in x_loads[1:]:
        x_load.start()
    for i in range(2, 5):
        load(i)
    loaded(0)

    spread = (
        lax.broadcasted_iota(jnp.int32, (RK, wide), 1) % RK
        == lax.broadcasted_iota(jnp.int32, (RK, wide), 0)
    ).astype(BF16)
    own_head = (
        lax.broadcasted_iota(jnp.int32, (cols, wide), 0) // HEAD
        == lax.broadcasted_iota(jnp.int32, (cols, wide), 1) // RK
    )
    diag = [
        jnp.where(
            own_head,
            lax.dot_general(basis[p], spread, (((0,), (0,)), ((), ())), preferred_element_type=F32),
            0.0,
        ).astype(BF16)
        for p in range(2)
    ]
    loaded(1)
    for p in range(2):
        small[:, p * wide : (p + 1) * wide] = jnp.dot(
            cot[p], diag[p], preferred_element_type=F32
        ).astype(BF16)

    def block(z, half):
        return pl.ds(pl.multiple_of((z * 2 + half) * rows, rows), rows)

    def first_copy(k, i, p):
        z = flip(at, order[k]) * pairs + i
        return remote(
            part.at[p, block(z, 1 - b)],
            arrived1.at[p, z],
            s1.at[p],
            r1.at[k * pairs + i, p],
            mate,
        )

    def multiply(here):
        sums = lax.dot_general(
            x[:, here], small[...], (((0,), (0,)), ((), ())), preferred_element_type=F32
        ).astype(BF16)
        for p in range(2):
            part[p, here] = sums[:, p * wide : (p + 1) * wide]

    apart = rows % 128 == 0
    for k in range(chunks):
        x_loads[k].wait()
        multiply(block(flip(at, order[k]), 1 - b) if apart else chunk_at(k))
        if k == 0:
            pl.semaphore_wait(barrier, outer + t - 1)
        for i in range(pairs):
            first_copy(k, i, 0).start()
    for k in range(chunks):
        for i in range(pairs):
            first_copy(k, i, 1).start()
    if apart:
        for k in range(chunks):
            multiply(block(flip(at, order[k]), b))

    def onward(k, p):
        for i in range(pairs):
            first_copy(k, i, p).wait_recv()
            if k < chunks - 1 or pairs > 1:
                z = flip(at, order[k]) * pairs + i
                send = remote(
                    summed.at[p, z], arrived2.at[p, a], s2.at[p], r2.at[p], (z * 2 + b, g)
                )
                summed[p, z] = (
                    part[p, block(z, b)].astype(F32) + arrived1[p, z].astype(F32)
                ).astype(BF16)
                if k < chunks - 1:
                    send.start()
                else:
                    pl.when(z != a)(send.start)

    def others(ref, p):
        return ref.at[p, pl.ds(0, outer - 1)]

    back = (((1,), (1,)), ((), ()))

    def gather(p):
        reduced = part[p, block(a, b)].astype(F32) + arrived1[p, a].astype(F32)
        remote(others(summed, p), others(arrived2, p), s2.at[p], r2.at[p], mate).wait_recv()
        for q in range(outer - 1, 0, -1):
            reduced = reduced + arrived2[p, flip(a, q)].astype(F32)
        if p == 0:
            for i in range(2, 5):
                loaded(i)
        moment = 0.9 * first[p] + 0.1 * reduced
        square = 0.95 * second[p] + 0.05 * reduced * reduced
        direction = moment / (jnp.sqrt(square) + 1e-08)
        tot[p, 0] = jnp.sum(direction * direction, axis=0, keepdims=True)

        def send_total(to):
            remote(tot.at[p, 0], tot_all.at[p, me], st.at[p], rt.at[p], to).start()

        def send_row(i, c):
            to = f + n // 2 + i
            to = to - n * (to // n)
            for h in range(t):
                send_total((to, h))
            return c

        lax.fori_loop(0, n // 2, send_row, 0)
        lax.fori_loop(n // 2 + 1, n, send_row, 0)
        for i in range(1, t):
            send_total((f, (g + i) % t))
        tot_all[p, me] = tot[p, 0]
        mom[p] = moment
        sqr[p] = square
        upper = direction.astype(BF16)
        lower = (direction - upper.astype(F32)).astype(BF16)
        raw[p] = lax.dot_general(upper, diag[p], back, preferred_element_type=F32) + lax.dot_general(
            lower, diag[p], back, preferred_element_type=F32
        )

    entries = depth * wide * t

    def all_totals(p):
        ref = tot_all.at[p, pl.ds(0, count - 1)]
        return remote(ref, ref, st.at[p], rt.at[p], mate)

    def piece(z, half, p, h):
        return copy.at[p, pl.ds(pl.multiple_of((z * 2 + half) * rows + h * bit, bit), bit)]

    def line_copy(z, p, h, sem, to):
        ref = piece(z, b, p, h)
        return remote(ref, ref, sem, rz.at[z, p, h], (to * 2 + b, g))

    def across(z, half, p, h):
        ref = piece(z, half, p, h)
        return remote(ref, ref, sy.at[p], ry.at[p], mate)

    def own_across(half, h):
        ref = piece(a, half, 1, h)
        return remote(ref, ref, sy.at[1], rm.at[h], mate)

    def crossed(p, blocks):
        ref = copy.at[p, pl.ds(0, blocks * rows)]
        return remote(ref, ref, sy.at[p], ry.at[p], mate)

    near = flip(a, 1)

    def beside(z, h):
        ref = piece(z, 1 - b, 1, h)
        return remote(ref, ref, sn.at[0], rn.at[0], (near * 2 + b, g))

    def whole_beside():
        ref = copy.at[1, block(a, b)]
        return remote(ref, ref, sn.at[0], rn.at[0], mate)

    def own_ways():
        for i, d in enumerate((2, -2, 1, -1)):
            yield i, d, a + d <= outer - 1 if d > 0 else a + d >= 0

    def finish(p):
        all_totals(p).wait_recv()
        mean = jnp.sum(jnp.sum(tot_all[p], axis=0), axis=1, keepdims=True) / entries
        scale = 1.0 / jnp.sqrt(mean + 0.25)
        move = scale * raw[p]
        fresh = w[p] - 0.1 * move
        copy[p, block(a, b)] = fresh.astype(BF16)
        for h in range(cut):
            for i, d, ok in own_ways():
                pl.when(ok)(line_copy(a, p, h, so.at[i, p], a + d).start)
            (own_across(b, h) if p else across(a, b, p, h)).start()
        step[p] = move
        new[p] = fresh

    def whole(z, p, sem):
        ref = copy.at[p, block(z, b)]
        return remote(ref, ref, sem, rn.at[0], mate)

    def relays(far):
        up = far > 0
        return (a < outer - 1 if up else a > 0), (sr.at[int(up), abs(far) - 2]), a + (1 if up else -1)

    def forward(d, p, h):
        for far in (d, -d):
            z = a - far

            def handle(far=far, z=z):
                line_copy(z, p, h, sn.at[0], a).wait_recv()
                if 2 <= d < outer - 1:
                    ok, sem, to = relays(far)
                    pl.when(ok)(line_copy(z, p, h, sem.at[p], to).start)
                if d == 1 and p == 1:
                    pl.when(z != near)(lambda: across(z, b, p, h).start())
                else:
                    across(z, b, p, h).start()

            pl.when(z >= 0 if far > 0 else z <= outer - 1)(handle)

    def sent(p):
        remote(arrived1.at[p], arrived1.at[p], s1.at[p], r1.at[0, p], mate).wait_send()
        remote(others(summed, p), others(arrived2, p), s2.at[p], r2.at[p], mate).wait_send()
        all_totals(p).wait_send()

    def sent_copies(p):
        for i, d, ok in own_ways():
            pl.when(ok)(whole(a, p, so.at[i, p]).wait_send)
        for d in range(2, outer - 1):
            for far in (d, -d):
                ok, sem, _ = relays(far)
                z = a - far
                there = z >= 0 if far > 0 else z <= outer - 1
                pl.when(jnp.logical_and(ok, there))(whole(z, p, sem.at[p]).wait_send)
        crossed(p, outer - p).wait_send()

    for k in range(chunks):
        onward(k, 0)
    onward(0, 1)
    gather(0)
    for k in range(1, chunks):
        onward(k, 1)
    gather(1)
    finish(0)

    def due(d, p, h):
        return 4.7 * p + (4.5 + 1.4 * h if d == 1 else 5.2 + 4 * (d - 2) + 3.8 * h)

    def pass_on(h):
        own_across(1 - b, h).wait_recv()
        beside(a, h).start()

    todo = [(4.6, lambda: finish(1)), (9, lambda: sent(0)), (9, lambda: sent(1))]
    for h in range(cut):
        for d in range(1, outer):
            for p in range(2):
                todo.append((due(d, p, h), functools.partial(forward, d, p, h)))
        todo.append((due(2, 1, h) + 0.1, functools.partial(pass_on, h)))
    todo.append((due(outer - 1, 1, cut - 1) - 0.1, lambda: sent_copies(0)))
    for _, act in sorted(todo, key=lambda item: item[0]):
        act()

    crossed(0, outer).wait_recv()
    if outer > 2:
        crossed(1, outer - 2).wait_recv()
    sent_copies(1)
    whole_beside().wait_recv()
    whole_beside().wait_send()


def store(step, new, copy, mom, sqr, *rest):
    outs, sem = rest[:10], rest[10]
    srcs = [ref.at[p] for ref in (step, new, copy, mom, sqr) for p in range(2)]
    order = (4, 5, 0, 1, 2, 3, 6, 7, 8, 9)
    moves = [pltpu.make_async_copy(srcs[i], outs[i], sem.at[i]) for i in order]
    for move in moves:
        move.start()
    for move in moves:
        move.wait()


def per_device(n, t, x, cq, cv, wq, wv, bq, bv, fq, sq, fv, sv):
    tokens, depth = x.shape
    rows, cols = wq.shape
    wide = fq.shape[1]
    outer = n // 2
    chunks = depth // max(2 * rows, min(depth, 256))
    cut = CUT if rows % (16 * CUT) == 0 else 1
    hbm = pl.BlockSpec(memory_space=pltpu.HBM)
    vmem = pl.BlockSpec(memory_space=pltpu.VMEM)
    shape = jax.ShapeDtypeStruct
    dma = pltpu.SemaphoreType.DMA
    kept = (
        pltpu.VMEM((2, rows, cols), F32),
        pltpu.VMEM((2, rows, cols), F32),
        pltpu.VMEM((2, depth, cols), BF16),
        pltpu.VMEM((2, rows, wide), F32),
        pltpu.VMEM((2, rows, wide), F32),
    )
    held = pl.pallas_call(
        functools.partial(body, n, t),
        out_shape=kept,
        in_specs=[hbm] * 11,
        out_specs=[vmem] * 5,
        scratch_shapes=[
            pltpu.VMEM((tokens, depth), BF16),
            pltpu.VMEM((2, tokens, cols), BF16),
            pltpu.VMEM((2, rows, cols), F32),
            pltpu.VMEM((2, RK, cols), BF16),
            pltpu.VMEM((2, rows, wide), F32),
            pltpu.VMEM((2, rows, wide), F32),
            pltpu.VMEM((tokens, 2 * wide), BF16),
            pltpu.VMEM((2, depth, wide), BF16),
            pltpu.VMEM((2, outer, rows, wide), BF16),
            pltpu.VMEM((2, outer, rows, wide), BF16),
            pltpu.VMEM((2, outer, rows, wide), BF16),
            pltpu.VMEM((2, rows, cols), F32),
            pltpu.VMEM((2, 1, 1, wide), F32),
            pltpu.VMEM((2, n * t, 1, wide), F32),
            dma((5,)),
            dma((chunks,)),
            dma((2,)),
            dma((outer, 2)),
            dma((2,)),
            dma((2,)),
            dma((2,)),
            dma((2,)),
            dma((4, 2)),
            dma((2, max(outer - 3, 1), 2)),
            dma((outer, 2, cut)),
            dma((2,)),
            dma((2,)),
            dma((1,)),
            dma((1,)),
            dma((cut,)),
        ],
        compiler_params=pltpu.CompilerParams(
            collective_id=0, has_side_effects=True, vmem_limit_bytes=62 * 10**6
        ),
        name="update",
    )(x, cq, cv, wq, wv, bq.T, bv.T, fq, sq, fv, sv)
    full, half = shape((rows, cols), F32), shape((rows, wide), F32)
    whole = shape((depth, cols), BF16)
    outs = pl.pallas_call(
        store,
        out_shape=(full,) * 4 + (whole,) * 2 + (half,) * 4,
        in_specs=[vmem] * 5,
        out_specs=[hbm] * 10,
        scratch_shapes=[dma((10,))],
        compiler_params=pltpu.CompilerParams(vmem_limit_bytes=40 * 2**20),
        name="store",
    )(*held)
    return tuple(outs[i] for i in (0, 1, 2, 3, 4, 5, 6, 8, 7, 9))


def solution(mesh):
    split = P("fs", "tp")
    return jax.shard_map(
        functools.partial(per_device, mesh.shape["fs"], mesh.shape["tp"]),
        mesh=mesh,
        in_specs=(P("fs", None),) + (split,) * 4 + (P("tp", None),) * 2 + (split,) * 4,
        out_specs=(split,) * 4 + (P(None, "tp"),) * 2 + (split,) * 4,
        check_vma=False,
    )
```

```python
import functools

import jax
import jax.numpy as jnp
from jax import lax
from jax.experimental import pallas as pl
from jax.experimental.pallas import tpu as pltpu
from jax.sharding import PartitionSpec as P

HEAD = 64
RK = 32
CUT = 2
FINE = 2
VSWAP = False
MESH = pl.DeviceIdType.MESH
END_PLAN = (
    ("finish", 0), ("own", "mate", 0, 1), ("own", "mate", 0, 0), ("gather", 1),
    ("own", "near", 0, 1), ("own", "far", 0, 0), ("pass", "near", 0, 1), ("own", "far", 0, 1),
    ("pass", "near", 0, 0), ("finish", 1), ("own", "mate", 1, 1), ("own", "mate", 1, 0),
    ("own", "far", 1, 0), ("own", "near", 0, 0), ("pass", "mid", 0, 0), ("own", "far", 1, 1),
    ("own", "near", 1, 1), ("pass", "end", 0, 0), ("own", "near", 1, 0), ("pass", "mid", 1, 0),
    ("pass", "near", 1, 1), ("beside", 0), ("pass", "end", 0, 1), ("pass", "end", 1, 0),
    ("beside", 1), ("pass", "mid", 0, 1), ("pass", "mid", 1, 1), ("pass", "end", 1, 1),
    ("pass", "near", 1, 0),
)
MIDDLE_PLAN = (
    ("finish", 0), ("own", "mate", 0, 0), ("own", "mate", 0, 1), ("gather", 1),
    ("own", "near", 0, 1), ("own", "inner", 0, 0), ("own", "near", 0, 0), ("pass", "inner", 0, 0),
    ("pass", "far", 0, 0), ("finish", 1), ("own", "far", 1, 0), ("own", "mate", 1, 0),
    ("own", "mate", 1, 1), ("own", "inner", 0, 1), ("own", "near", 1, 1), ("pass", "near", 0, 1),
    ("pass", "far", 0, 1), ("pass", "far", 1, 0), ("own", "inner", 1, 0), ("pass", "inner", 0, 1),
    ("own", "far", 1, 1), ("own", "inner", 1, 1), ("pass", "far", 1, 1), ("pass", "near", 1, 0),
    ("pass", "near", 0, 0), ("pass", "near", 1, 1), ("own", "near", 1, 0), ("beside", 1),
    ("pass", "inner", 1, 0), ("beside", 0), ("pass", "inner", 1, 1),
)
MIDDLE_RELAYS = (True, False)
F32 = jnp.float32
BF16 = jnp.bfloat16


def flip(x, bits):
    out, weight = x, 1
    while weight <= bits:
        if bits & weight:
            out = out + weight * (1 - 2 * ((x // weight) % 2))
        weight *= 2
    return out


def remote(src, dst, send, recv, to):
    return pltpu.make_async_remote_copy(
        src_ref=src, dst_ref=dst, send_sem=send, recv_sem=recv, device_id=to, device_id_type=MESH
    )


def body(
    n,
    t,
    x_hbm,
    cq_hbm,
    cv_hbm,
    wq_hbm,
    wv_hbm,
    bq_hbm,
    bv_hbm,
    fq_hbm,
    sq_hbm,
    fv_hbm,
    sv_hbm,
    step,
    new,
    copy,
    mom,
    sqr,
    x,
    cot,
    w,
    basis,
    first,
    second,
    small,
    part,
    summed,
    arrived1,
    arrived2,
    raw,
    tot,
    tot_all,
    in_sem,
    x_sem,
    s1,
    r1,
    s2,
    r2,
    st,
    rt,
    so,
    sr,
    rz,
    sy,
    ry,
    sn,
    rn,
    rm,
    line,
):
    f = lax.axis_index("fs")
    g = lax.axis_index("tp")
    me = f * t + g
    count = n * t
    outer = n // 2
    a, b = f // 2, f % 2
    mate = (a * 2 + 1 - b, g)
    depth = x.shape[1]
    rows = depth // n
    cols = w.shape[2]
    wide = cols // HEAD * RK
    cut = rz.shape[2]
    planned = outer == 4 and cut == CUT
    bit = rows // cut
    fine = r1.shape[2]
    slip = rows // fine

    chunk = max(2 * rows, min(depth, 256))
    chunks = depth // chunk
    pairs = chunk // (2 * rows)
    order = list(range(chunks // 2, chunks)) + list(range(chunks // 2 - 1, -1, -1))
    at = a // pairs

    def chunk_at(k):
        return pl.ds(pl.multiple_of(flip(at, order[k]) * chunk, chunk), chunk)

    sources = ((bq_hbm, bv_hbm), (cq_hbm, cv_hbm), (fq_hbm, fv_hbm), (sq_hbm, sv_hbm), (wq_hbm, wv_hbm))
    holders = (basis, cot, first, second, w)

    def load(i):
        for p in range(2):
            pltpu.make_async_copy(sources[i][p], holders[i].at[p], in_sem.at[i]).start()

    def loaded(i):
        pltpu.make_async_copy(holders[i], holders[i], in_sem.at[i]).wait()

    x_loads = [
        pltpu.make_async_copy(x_hbm.at[:, chunk_at(k)], x.at[:, chunk_at(k)], x_sem.at[k])
        for k in range(chunks)
    ]
    load(0)
    load(1)
    x_loads[0].start()

    barrier = pltpu.get_barrier_semaphore()

    def hello(to):
        pl.semaphore_signal(barrier, inc=1, device_id=to, device_id_type=MESH)

    def at_line(z):
        return (z * 2 + b, g)

    def greet_line(i, c):
        hello(at_line((a + 1 + i) % outer))
        return c

    chained = outer <= 8
    below, above = a > 0, a < outer - 1
    hello(mate)
    if chained:
        pl.when(below)(lambda: hello(at_line(a - 1)))
        pl.when(above)(lambda: hello(at_line(a + 1)))
        near_by = below.astype(jnp.int32) + above.astype(jnp.int32)
    else:
        lax.fori_loop(0, outer - 1, greet_line, 0)
        near_by = outer - 1
    for i in range(1, t):
        hello((f, (g + i) % t))

    def tell(way, z):
        pl.semaphore_signal(
            line.at[way], inc=1, device_id=at_line(z), device_id_type=MESH
        )

    def tell_neighbours():
        if chained:

            @pl.when(jnp.logical_and(below, above))
            def _():
                tell(0, a - 1)
                tell(1, a + 1)

    def hear(start, stop):
        if chained:
            for way, number, go, to in (
                (0, outer - 2 - a, below, a - 1),
                (1, a - 1, above, a + 1),
            ):

                def pass_along(i, c, way=way, go=go, to=to):
                    pl.semaphore_wait(line.at[way], 1)
                    pl.when(go)(lambda: tell(way, to))
                    return c

                lax.fori_loop(start, jnp.clip(number, start, stop), pass_along, 0)

    for x_load in x_loads[1:]:
        x_load.start()
    for i in range(2, 5):
        load(i)
    loaded(0)

    spread = (
        lax.broadcasted_iota(jnp.int32, (RK, wide), 1) % RK
        == lax.broadcasted_iota(jnp.int32, (RK, wide), 0)
    ).astype(BF16)
    own_head = (
        lax.broadcasted_iota(jnp.int32, (cols, wide), 0) // HEAD
        == lax.broadcasted_iota(jnp.int32, (cols, wide), 1) // RK
    )
    diag = [
        jnp.where(
            own_head,
            lax.dot_general(basis[p], spread, (((0,), (0,)), ((), ())), preferred_element_type=F32),
            0.0,
        ).astype(BF16)
        for p in range(2)
    ]
    loaded(1)
    for p in range(2):
        small[:, p * wide : (p + 1) * wide] = jnp.dot(
            cot[p], diag[p], preferred_element_type=F32
        ).astype(BF16)

    def block(z, half):
        return pl.ds(pl.multiple_of((z * 2 + half) * rows, rows), rows)

    def first_copy(k, i, p, h):
        z = flip(at, order[k]) * pairs + i
        there = pl.ds(h * slip, slip)
        return remote(
            part.at[p, pl.ds(pl.multiple_of((z * 2 + 1 - b) * rows + h * slip, slip), slip)],
            arrived1.at[p, z, there],
            s1.at[p],
            r1.at[k * pairs + i, p, h],
            mate,
        )

    def first_starts(k, p):
        for i in range(pairs):
            for h in range(fine):
                first_copy(k, i, p, h).start()

    def multiply(here):
        sums = lax.dot_general(
            x[:, here], small[...], (((0,), (0,)), ((), ())), preferred_element_type=F32
        ).astype(BF16)
        for p in range(2):
            part[p, here] = sums[:, p * wide : (p + 1) * wide]

    apart = rows % 128 == 0
    order_of = (list(range(chunks)), list(range(chunks)))
    if VSWAP and chunks == 4:
        order_of = (order_of[0], [2, 0, 1, 3])
    for k in range(chunks):
        x_loads[k].wait()
        multiply(block(flip(at, order[k]), 1 - b) if apart else chunk_at(k))
        if k == 0:
            pl.semaphore_wait(barrier, near_by + t)
        first_starts(k, 0)
        if k == 0:
            tell_neighbours()
    for k in order_of[1]:
        first_starts(k, 1)
    hear(0, 1)
    if apart:
        for k in range(chunks):
            multiply(block(flip(at, order[k]), b))

    def onward(k, p):
        for i in range(pairs):
            z = flip(at, order[k]) * pairs + i
            for h in range(fine):
                first_copy(k, i, p, h).wait_recv()
                if k < chunks - 1 or pairs > 1:
                    there = pl.ds(h * slip, slip)
                    send = remote(
                        summed.at[p, z, there],
                        arrived2.at[p, a, there],
                        s2.at[p],
                        r2.at[p],
                        (z * 2 + b, g),
                    )
                    mine = pl.ds(pl.multiple_of((z * 2 + b) * rows + h * slip, slip), slip)
                    summed[p, z, there] = (
                        part[p, mine].astype(F32) + arrived1[p, z, there].astype(F32)
                    ).astype(BF16)
                    if k < chunks - 1:
                        send.start()
                    else:
                        pl.when(z != a)(send.start)

    def others(ref, p):
        return ref.at[p, pl.ds(0, outer - 1)]

    back = (((1,), (1,)), ((), ()))

    def gather(p):
        reduced = part[p, block(a, b)].astype(F32) + arrived1[p, a].astype(F32)
        remote(others(summed, p), others(arrived2, p), s2.at[p], r2.at[p], mate).wait_recv()
        for q in range(outer - 1, 0, -1):
            reduced = reduced + arrived2[p, flip(a, q)].astype(F32)
        if p == 0:
            for i in range(2, 5):
                loaded(i)
        moment = 0.9 * first[p] + 0.1 * reduced
        square = 0.95 * second[p] + 0.05 * reduced * reduced
        direction = moment / (jnp.sqrt(square) + 1e-08)
        tot[p, 0] = jnp.sum(direction * direction, axis=0, keepdims=True)

        def send_total(to):
            remote(tot.at[p, 0], tot_all.at[p, me], st.at[p], rt.at[p], to).start()

        def send_row(i, c):
            to = f + n // 2 + i
            to = to - n * (to // n)
            for h in range(t):
                send_total((to, h))
            return c

        lax.fori_loop(0, n // 2, send_row, 0)
        lax.fori_loop(n // 2 + 1, n, send_row, 0)
        for i in range(1, t):
            send_total((f, (g + i) % t))
        tot_all[p, me] = tot[p, 0]
        mom[p] = moment
        sqr[p] = square
        upper = direction.astype(BF16)
        lower = (direction - upper.astype(F32)).astype(BF16)
        raw[p] = lax.dot_general(upper, diag[p], back, preferred_element_type=F32) + lax.dot_general(
            lower, diag[p], back, preferred_element_type=F32
        )

    entries = depth * wide * t

    def all_totals(p):
        ref = tot_all.at[p, pl.ds(0, count - 1)]
        return remote(ref, ref, st.at[p], rt.at[p], mate)

    def piece(z, half, p, h):
        return copy.at[p, pl.ds(pl.multiple_of((z * 2 + half) * rows + h * bit, bit), bit)]

    def line_copy(z, p, h, sem, to):
        ref = piece(z, b, p, h)
        return remote(ref, ref, sem, rz.at[z, p, h], (to * 2 + b, g))

    def across(z, half, p, h):
        ref = piece(z, half, p, h)
        return remote(ref, ref, sy.at[p], ry.at[p], mate)

    def own_across(half, h):
        ref = piece(a, half, 1, h)
        return remote(ref, ref, sy.at[1], rm.at[h], mate)

    def crossed(p, blocks):
        ref = copy.at[p, pl.ds(0, blocks * rows)]
        return remote(ref, ref, sy.at[p], ry.at[p], mate)

    near = flip(a, 1)

    def beside(z, h):
        ref = piece(z, 1 - b, 1, h)
        return remote(ref, ref, sn.at[0], rn.at[0], (near * 2 + b, g))

    def whole_beside():
        ref = copy.at[1, block(a, b)]
        return remote(ref, ref, sn.at[0], rn.at[0], mate)

    def own_ways():
        for i, d in enumerate((2, -2, 1, -1)):
            yield i, d, a + d <= outer - 1 if d > 0 else a + d >= 0

    def scaled(p):
        all_totals(p).wait_recv()
        mean = jnp.sum(jnp.sum(tot_all[p], axis=0), axis=1, keepdims=True) / entries
        scale = 1.0 / jnp.sqrt(mean + 0.25)
        move = scale * raw[p]
        fresh = w[p] - 0.1 * move
        copy[p, block(a, b)] = fresh.astype(BF16)

        def keep():
            step[p] = move
            new[p] = fresh

        return keep

    def finish(p):
        keep = scaled(p)
        for h in range(cut):
            for i, d, ok in own_ways():
                pl.when(ok)(line_copy(a, p, h, so.at[i, p], a + d).start)
            (own_across(b, h) if p else across(a, b, p, h)).start()
        keep()

    def whole(z, p, sem):
        ref = copy.at[p, block(z, b)]
        return remote(ref, ref, sem, rn.at[0], mate)

    def relays(far):
        up = far > 0
        return (a < outer - 1 if up else a > 0), (sr.at[int(up), abs(far) - 2]), a + (1 if up else -1)

    def forward(d, p, h):
        for far in (d, -d):
            z = a - far

            def handle(far=far, z=z):
                line_copy(z, p, h, sn.at[0], a).wait_recv()
                if 2 <= d < outer - 1:
                    ok, sem, to = relays(far)
                    pl.when(ok)(line_copy(z, p, h, sem.at[p], to).start)
                if d == 1 and p == 1:
                    pl.when(z != near)(lambda: across(z, b, p, h).start())
                else:
                    across(z, b, p, h).start()

            pl.when(z >= 0 if far > 0 else z <= outer - 1)(handle)

    def sent(p):
        remote(arrived1.at[p], arrived1.at[p], s1.at[p], rn.at[0], mate).wait_send()
        remote(others(summed, p), others(arrived2, p), s2.at[p], r2.at[p], mate).wait_send()
        all_totals(p).wait_send()

    def sent_copies(p):
        for i, d, ok in own_ways():
            pl.when(ok)(whole(a, p, so.at[i, p]).wait_send)
        for d in range(2, outer - 1):
            for far in (d, -d):
                ok, sem, _ = relays(far)
                z = a - far
                there = z >= 0 if far > 0 else z <= outer - 1
                pl.when(jnp.logical_and(ok, there))(whole(z, p, sem.at[p]).wait_send)
        crossed(p, outer - p).wait_send()

    onward(0, 0)
    hear(1, outer)
    for k in range(1, chunks):
        onward(k, 0)
    onward(order_of[1][0], 1)
    gather(0)
    for k in order_of[1][1:]:
        onward(k, 1)
    def play(plan, inward, at_end):
        later = []
        away = {"near": 1, "mid": 2, "end": 3} if at_end else {"near": -1, "inner": 1, "far": 2}
        reach = dict(away, far=2)
        for i, (kind, *rest) in enumerate(plan):
            if kind in ("pass", "beside") or i == len(plan) - 1:
                while later:
                    later.pop()()
            if i == len(plan) - 3:
                sent(0)
                sent(1)
            if kind == "gather":
                gather(1)
            elif kind == "finish":
                later.append(scaled(rest[0]))
            elif kind == "beside":
                own_across(1 - b, rest[0]).wait_recv()
                beside(a, rest[0]).start()
            elif rest[0] == "mate":
                _, p, h = rest
                (own_across(b, h) if p else across(a, b, p, h)).start()
            elif kind == "own":
                way, p, h = rest
                line_copy(a, p, h, so.at[0, p], a + inward * reach[way]).start()
            else:
                way, p, h = rest
                z = a + inward * away[way]
                line_copy(z, p, h, sn.at[0], a).wait_recv()
                if not at_end and (way == "far" or way == "inner" and MIDDLE_RELAYS[p]):
                    line_copy(z, p, h, so.at[0, p], a - inward).start()
                if p == 0 or way != "near":
                    across(z, b, p, h).start()

    def z_sent(p):
        for blocks, here in ((2, at_end), (4, jnp.logical_not(at_end))):
            ref = copy.at[p, pl.ds(0, blocks * rows)]
            pl.when(here)(remote(ref, ref, so.at[0, p], rn.at[0], mate).wait_send)

    if planned:
        inward = jnp.where(a < outer // 2, 1, -1)
        at_end = jnp.logical_or(a == 0, a == outer - 1)
        pl.when(at_end)(lambda: play(END_PLAN, inward, True))
        pl.when(jnp.logical_not(at_end))(lambda: play(MIDDLE_PLAN, inward, False))
        z_sent(0)
        crossed(0, outer).wait_send()
        crossed(0, outer).wait_recv()
        crossed(1, outer - 2).wait_recv()
        z_sent(1)
        crossed(1, outer - 1).wait_send()
    else:
        gather(1)
        finish(0)

        def due(d, p, h):
            return 4.7 * p + (4.5 + 1.4 * h if d == 1 else 5.2 + 4 * (d - 2) + 3.8 * h)

        def pass_on(h):
            own_across(1 - b, h).wait_recv()
            beside(a, h).start()

        todo = [(4.6, lambda: finish(1)), (9, lambda: sent(0)), (9, lambda: sent(1))]
        for h in range(cut):
            for d in range(1, outer):
                for p in range(2):
                    todo.append((due(d, p, h), functools.partial(forward, d, p, h)))
            todo.append((due(2, 1, h) + 0.1, functools.partial(pass_on, h)))
        todo.append((due(outer - 1, 1, cut - 1) - 0.1, lambda: sent_copies(0)))
        for _, act in sorted(todo, key=lambda item: item[0]):
            act()
        crossed(0, outer).wait_recv()
        if outer > 2:
            crossed(1, outer - 2).wait_recv()
        sent_copies(1)
    whole_beside().wait_recv()
    whole_beside().wait_send()


def store(step, new, copy, mom, sqr, *rest):
    outs, sem = rest[:10], rest[10]
    srcs = [ref.at[p] for ref in (step, new, copy, mom, sqr) for p in range(2)]
    order = (4, 5, 0, 1, 2, 3, 6, 7, 8, 9)
    moves = [pltpu.make_async_copy(srcs[i], outs[i], sem.at[i]) for i in order]
    for move in moves:
        move.start()
    for move in moves:
        move.wait()


def per_device(n, t, x, cq, cv, wq, wv, bq, bv, fq, sq, fv, sv):
    tokens, depth = x.shape
    rows, cols = wq.shape
    wide = fq.shape[1]
    outer = n // 2
    chunks = depth // max(2 * rows, min(depth, 256))
    cut = CUT if rows % (16 * CUT) == 0 else 1
    planned = outer == 4 and cut == CUT
    fine = FINE if rows % (16 * FINE) == 0 else 1
    hbm = pl.BlockSpec(memory_space=pltpu.HBM)
    vmem = pl.BlockSpec(memory_space=pltpu.VMEM)
    shape = jax.ShapeDtypeStruct
    dma = pltpu.SemaphoreType.DMA
    kept = (
        pltpu.VMEM((2, rows, cols), F32),
        pltpu.VMEM((2, rows, cols), F32),
        pltpu.VMEM((2, depth, cols), BF16),
        pltpu.VMEM((2, rows, wide), F32),
        pltpu.VMEM((2, rows, wide), F32),
    )
    held = pl.pallas_call(
        functools.partial(body, n, t),
        out_shape=kept,
        in_specs=[hbm] * 11,
        out_specs=[vmem] * 5,
        scratch_shapes=[
            pltpu.VMEM((tokens, depth), BF16),
            pltpu.VMEM((2, tokens, cols), BF16),
            pltpu.VMEM((2, rows, cols), F32),
            pltpu.VMEM((2, RK, cols), BF16),
            pltpu.VMEM((2, rows, wide), F32),
            pltpu.VMEM((2, rows, wide), F32),
            pltpu.VMEM((tokens, 2 * wide), BF16),
            pltpu.VMEM((2, depth, wide), BF16),
            pltpu.VMEM((2, outer, rows, wide), BF16),
            pltpu.VMEM((2, outer, rows, wide), BF16),
            pltpu.VMEM((2, outer, rows, wide), BF16),
            pltpu.VMEM((2, rows, cols), F32),
            pltpu.VMEM((2, 1, 1, wide), F32),
            pltpu.VMEM((2, n * t, 1, wide), F32),
            dma((5,)),
            dma((chunks,)),
            dma((2,)),
            dma((outer, 2, fine)),
            dma((2,)),
            dma((2,)),
            dma((2,)),
            dma((2,)),
            dma((1 if planned else 4, 2)),
            dma((1, 1, 1) if planned else (2, max(outer - 3, 1), 2)),
            dma((outer, 2, cut)),
            dma((2,)),
            dma((2,)),
            dma((1,)),
            dma((1,)),
            dma((cut,)),
            pltpu.SemaphoreType.REGULAR((2,)),
        ],
        compiler_params=pltpu.CompilerParams(
            collective_id=0, has_side_effects=True, vmem_limit_bytes=62 * 10**6
        ),
        name="update",
    )(x, cq, cv, wq, wv, bq.T, bv.T, fq, sq, fv, sv)
    full, half = shape((rows, cols), F32), shape((rows, wide), F32)
    whole = shape((depth, cols), BF16)
    outs = pl.pallas_call(
        store,
        out_shape=(full,) * 4 + (whole,) * 2 + (half,) * 4,
        in_specs=[vmem] * 5,
        out_specs=[hbm] * 10,
        scratch_shapes=[dma((10,))],
        compiler_params=pltpu.CompilerParams(vmem_limit_bytes=40 * 2**20),
        name="store",
    )(*held)
    return tuple(outs[i] for i in (0, 1, 2, 3, 4, 5, 6, 8, 7, 9))


def solution(mesh):
    split = P("fs", "tp")
    return jax.shard_map(
        functools.partial(per_device, mesh.shape["fs"], mesh.shape["tp"]),
        mesh=mesh,
        in_specs=(P("fs", None),) + (split,) * 4 + (P("tp", None),) * 2 + (split,) * 4,
        out_specs=(split,) * 4 + (P(None, "tp"),) * 2 + (split,) * 4,
        check_vma=False,
    )
```

```python
import functools

import jax
import jax.numpy as jnp
from jax import lax
from jax.experimental import pallas as pl
from jax.experimental.pallas import tpu as pltpu
from jax.sharding import PartitionSpec as P

HEAD = 64
RK = 32
CUT = 2
MESH = pl.DeviceIdType.MESH
END_PLAN = (
    ("finish", 0), ("own", "near", 0, 0), ("own", "mate", 0, 1), ("own", "mate", 0, 0),
    ("gather", 1), ("own", "near", 0, 1), ("pass", "near", 0, 1), ("own", "far", 0, 1),
    ("pass", "near", 0, 0), ("own", "far", 0, 0), ("pass", "mid", 0, 0), ("finish", 1),
    ("own", "mate", 1, 0), ("own", "mate", 1, 1), ("own", "far", 1, 1), ("own", "far", 1, 0),
    ("pass", "mid", 0, 1), ("own", "near", 1, 1), ("pass", "end", 0, 1), ("pass", "mid", 1, 1),
    ("pass", "mid", 1, 0), ("own", "near", 1, 0), ("pass", "near", 1, 0), ("pass", "end", 1, 1),
    ("beside", 1), ("pass", "end", 0, 0), ("beside", 0), ("pass", "end", 1, 0),
    ("pass", "near", 1, 1),
)
MIDDLE_PLAN = (
    ("finish", 0), ("own", "inner", 0, 0), ("own", "near", 0, 1), ("own", "mate", 0, 1),
    ("own", "inner", 0, 1), ("own", "mate", 0, 0), ("own", "near", 0, 0), ("gather", 1),
    ("pass", "inner", 0, 0), ("pass", "inner", 0, 1), ("pass", "near", 0, 1),
    ("pass", "near", 0, 0), ("finish", 1), ("own", "far", 1, 1), ("pass", "far", 0, 1),
    ("own", "near", 1, 0), ("own", "mate", 1, 0), ("own", "far", 1, 0), ("pass", "far", 0, 0),
    ("own", "mate", 1, 1), ("pass", "far", 1, 1), ("pass", "far", 1, 0), ("own", "inner", 1, 0),
    ("pass", "near", 1, 1), ("own", "inner", 1, 1), ("own", "near", 1, 1), ("beside", 0),
    ("pass", "inner", 1, 0), ("pass", "inner", 1, 1), ("beside", 1), ("pass", "near", 1, 0),
)
MIDDLE_RELAYS = (True, False)
F32 = jnp.float32
BF16 = jnp.bfloat16


def flip(x, bits):
    out, weight = x, 1
    while weight <= bits:
        if bits & weight:
            out = out + weight * (1 - 2 * ((x // weight) % 2))
        weight *= 2
    return out


def remote(src, dst, send, recv, to):
    return pltpu.make_async_remote_copy(
        src_ref=src, dst_ref=dst, send_sem=send, recv_sem=recv, device_id=to, device_id_type=MESH
    )


def body(
    n,
    t,
    x_hbm,
    cq_hbm,
    cv_hbm,
    wq_hbm,
    wv_hbm,
    bq_hbm,
    bv_hbm,
    fq_hbm,
    sq_hbm,
    fv_hbm,
    sv_hbm,
    step,
    new,
    copy,
    mom,
    sqr,
    x,
    cot,
    w,
    basis,
    first,
    second,
    small,
    part,
    summed,
    arrived1,
    arrived2,
    raw,
    tot,
    tot_all,
    in_sem,
    x_sem,
    s1,
    r1,
    s2,
    r2,
    st,
    rt,
    so,
    sr,
    sy,
    ry,
    sn,
    rn,
    rm,
    line,
):
    f = lax.axis_index("fs")
    g = lax.axis_index("tp")
    me = f * t + g
    count = n * t
    outer = n // 2
    a, b = f // 2, f % 2
    mate = (a * 2 + 1 - b, g)
    depth = x.shape[1]
    rows = depth // n
    cols = w.shape[2]
    wide = cols // HEAD * RK
    cut = r1.shape[2]
    rz = r1
    planned = outer == 4 and cut == CUT
    bit = rows // cut
    fine = r1.shape[2]
    slip = rows // fine

    chunk = max(2 * rows, min(depth, 256))
    chunks = depth // chunk
    pairs = chunk // (2 * rows)
    order = list(range(chunks // 2, chunks)) + list(range(chunks // 2 - 1, -1, -1))
    at = a // pairs

    def chunk_at(k):
        return pl.ds(pl.multiple_of(flip(at, order[k]) * chunk, chunk), chunk)

    sources = ((bq_hbm, bv_hbm), (cq_hbm, cv_hbm), (fq_hbm, fv_hbm), (sq_hbm, sv_hbm), (wq_hbm, wv_hbm))
    holders = (basis, cot, first, second, w)

    def load(i):
        for p in range(2):
            pltpu.make_async_copy(sources[i][p], holders[i].at[p], in_sem.at[i]).start()

    def loaded(i):
        pltpu.make_async_copy(holders[i], holders[i], in_sem.at[i]).wait()

    x_loads = [
        pltpu.make_async_copy(x_hbm.at[:, chunk_at(k)], x.at[:, chunk_at(k)], x_sem.at[k])
        for k in range(chunks)
    ]
    load(0)
    load(1)
    x_loads[0].start()

    barrier = pltpu.get_barrier_semaphore()

    def hello(to):
        pl.semaphore_signal(barrier, inc=1, device_id=to, device_id_type=MESH)

    def at_line(z):
        return (z * 2 + b, g)

    def greet_line(i, c):
        hello(at_line((a + 1 + i) % outer))
        return c

    chained = outer <= 8
    below, above = a > 0, a < outer - 1
    hello(mate)
    if chained:
        pl.when(below)(lambda: hello(at_line(a - 1)))
        pl.when(above)(lambda: hello(at_line(a + 1)))
        near_by = below.astype(jnp.int32) + above.astype(jnp.int32)
    else:
        lax.fori_loop(0, outer - 1, greet_line, 0)
        near_by = outer - 1
    for i in range(1, t):
        hello((f, (g + i) % t))

    def tell(way, z):
        pl.semaphore_signal(
            line.at[way], inc=1, device_id=at_line(z), device_id_type=MESH
        )

    def tell_neighbours():
        if chained:

            @pl.when(jnp.logical_and(below, above))
            def _():
                tell(0, a - 1)
                tell(1, a + 1)

    def hear(start, stop):
        if chained:
            for way, number, go, to in (
                (0, outer - 2 - a, below, a - 1),
                (1, a - 1, above, a + 1),
            ):

                def pass_along(i, c, way=way, go=go, to=to):
                    pl.semaphore_wait(line.at[way], 1)
                    pl.when(go)(lambda: tell(way, to))
                    return c

                lax.fori_loop(start, jnp.clip(number, start, stop), pass_along, 0)

    for x_load in x_loads[1:]:
        x_load.start()
    for i in range(2, 5):
        load(i)
    loaded(0)

    spread = (
        lax.broadcasted_iota(jnp.int32, (RK, wide), 1) % RK
        == lax.broadcasted_iota(jnp.int32, (RK, wide), 0)
    ).astype(BF16)
    own_head = (
        lax.broadcasted_iota(jnp.int32, (cols, wide), 0) // HEAD
        == lax.broadcasted_iota(jnp.int32, (cols, wide), 1) // RK
    )
    diag = [
        jnp.where(
            own_head,
            lax.dot_general(basis[p], spread, (((0,), (0,)), ((), ())), preferred_element_type=F32),
            0.0,
        ).astype(BF16)
        for p in range(2)
    ]
    loaded(1)
    for p in range(2):
        small[:, p * wide : (p + 1) * wide] = jnp.dot(
            cot[p], diag[p], preferred_element_type=F32
        ).astype(BF16)

    def block(z, half):
        return pl.ds(pl.multiple_of((z * 2 + half) * rows, rows), rows)

    def first_copy(k, i, p, h):
        z = flip(at, order[k]) * pairs + i
        there = pl.ds(h * slip, slip)
        return remote(
            part.at[p, pl.ds(pl.multiple_of((z * 2 + 1 - b) * rows + h * slip, slip), slip)],
            arrived1.at[p, z, there],
            s1.at[p],
            r1.at[k * pairs + i, p, h],
            mate,
        )

    def first_starts(k, p):
        for i in range(pairs):
            for h in range(fine):
                first_copy(k, i, p, h).start()

    def multiply(here):
        sums = lax.dot_general(
            x[:, here], small[...], (((0,), (0,)), ((), ())), preferred_element_type=F32
        ).astype(BF16)
        for p in range(2):
            part[p, here] = sums[:, p * wide : (p + 1) * wide]

    apart = rows % 128 == 0
    order_of = (list(range(chunks)), list(range(chunks)))
    if chunks == 4:
        order_of = (order_of[0], [0, 2, 1, 3])
    for k in range(chunks):
        x_loads[k].wait()
        multiply(block(flip(at, order[k]), 1 - b) if apart else chunk_at(k))
        if k == 0:
            pl.semaphore_wait(barrier, near_by + t)
        first_starts(k, 0)
        if k == 0:
            tell_neighbours()
    for k in order_of[1]:
        first_starts(k, 1)
    hear(0, 1)
    if apart:
        for k in range(chunks):
            multiply(block(flip(at, order[k]), b))

    def onward(k, p):
        for i in range(pairs):
            z = flip(at, order[k]) * pairs + i
            for h in range(fine):
                first_copy(k, i, p, h).wait_recv()
                if k < chunks - 1 or pairs > 1:
                    there = pl.ds(h * slip, slip)
                    send = remote(
                        summed.at[p, z, there],
                        arrived2.at[p, a, there],
                        s2.at[p],
                        r2.at[p],
                        (z * 2 + b, g),
                    )
                    mine = pl.ds(pl.multiple_of((z * 2 + b) * rows + h * slip, slip), slip)
                    summed[p, z, there] = (
                        part[p, mine].astype(F32) + arrived1[p, z, there].astype(F32)
                    ).astype(BF16)
                    if k < chunks - 1:
                        send.start()
                    else:
                        pl.when(z != a)(send.start)

    def others(ref, p):
        return ref.at[p, pl.ds(0, outer - 1)]

    back = (((1,), (1,)), ((), ()))

    def gather(p):
        reduced = part[p, block(a, b)].astype(F32) + arrived1[p, a].astype(F32)
        remote(others(summed, p), others(arrived2, p), s2.at[p], r2.at[p], mate).wait_recv()
        for q in range(outer - 1, 0, -1):
            reduced = reduced + arrived2[p, flip(a, q)].astype(F32)
        if p == 0:
            for i in range(2, 5):
                loaded(i)
        moment = 0.9 * first[p] + 0.1 * reduced
        square = 0.95 * second[p] + 0.05 * reduced * reduced
        direction = moment / (jnp.sqrt(square) + 1e-08)
        tot[p, 0] = jnp.sum(direction * direction, axis=0, keepdims=True)

        def send_total(to):
            remote(tot.at[p, 0], tot_all.at[p, me], st.at[p], rt.at[p], to).start()

        def send_row(i, c):
            to = f + n // 2 + i
            to = to - n * (to // n)
            for h in range(t):
                send_total((to, h))
            return c

        lax.fori_loop(0, n // 2, send_row, 0)
        lax.fori_loop(n // 2 + 1, n, send_row, 0)
        for i in range(1, t):
            send_total((f, (g + i) % t))
        tot_all[p, me] = tot[p, 0]
        mom[p] = moment
        sqr[p] = square
        upper = direction.astype(BF16)
        lower = (direction - upper.astype(F32)).astype(BF16)
        raw[p] = lax.dot_general(upper, diag[p], back, preferred_element_type=F32) + lax.dot_general(
            lower, diag[p], back, preferred_element_type=F32
        )

    entries = depth * wide * t

    def all_totals(p):
        ref = tot_all.at[p, pl.ds(0, count - 1)]
        return remote(ref, ref, st.at[p], rt.at[p], mate)

    def piece(z, half, p, h):
        return copy.at[p, pl.ds(pl.multiple_of((z * 2 + half) * rows + h * bit, bit), bit)]

    def line_copy(z, p, h, sem, to):
        ref = piece(z, b, p, h)
        return remote(ref, ref, sem, rz.at[z, p, h], (to * 2 + b, g))

    def across(z, half, p, h):
        ref = piece(z, half, p, h)
        return remote(ref, ref, sy.at[p], ry.at[p], mate)

    def own_across(half, h):
        ref = piece(a, half, 1, h)
        return remote(ref, ref, sy.at[1], rm.at[h], mate)

    def crossed(p, blocks):
        ref = copy.at[p, pl.ds(0, blocks * rows)]
        return remote(ref, ref, sy.at[p], ry.at[p], mate)

    near = flip(a, 1)

    def beside(z, h):
        ref = piece(z, 1 - b, 1, h)
        return remote(ref, ref, sn.at[0], rn.at[0], (near * 2 + b, g))

    def whole_beside():
        ref = copy.at[1, block(a, b)]
        return remote(ref, ref, sn.at[0], rn.at[0], mate)

    def own_ways():
        for i, d in enumerate((2, -2, 1, -1)):
            yield i, d, a + d <= outer - 1 if d > 0 else a + d >= 0

    def scaled(p):
        all_totals(p).wait_recv()
        mean = jnp.sum(jnp.sum(tot_all[p], axis=0), axis=1, keepdims=True) / entries
        scale = 1.0 / jnp.sqrt(mean + 0.25)
        move = scale * raw[p]
        fresh = w[p] - 0.1 * move
        copy[p, block(a, b)] = fresh.astype(BF16)

        def keep():
            step[p] = move
            new[p] = fresh

        return keep

    def finish(p):
        keep = scaled(p)
        for h in range(cut):
            for i, d, ok in own_ways():
                pl.when(ok)(line_copy(a, p, h, so.at[i, p], a + d).start)
            (own_across(b, h) if p else across(a, b, p, h)).start()
        keep()

    def whole(z, p, sem):
        ref = copy.at[p, block(z, b)]
        return remote(ref, ref, sem, rn.at[0], mate)

    def relays(far):
        up = far > 0
        return (a < outer - 1 if up else a > 0), (sr.at[int(up), abs(far) - 2]), a + (1 if up else -1)

    def forward(d, p, h):
        for far in (d, -d):
            z = a - far

            def handle(far=far, z=z):
                line_copy(z, p, h, sn.at[0], a).wait_recv()
                if 2 <= d < outer - 1:
                    ok, sem, to = relays(far)
                    pl.when(ok)(line_copy(z, p, h, sem.at[p], to).start)
                if d == 1 and p == 1:
                    pl.when(z != near)(lambda: across(z, b, p, h).start())
                else:
                    across(z, b, p, h).start()

            pl.when(z >= 0 if far > 0 else z <= outer - 1)(handle)

    def sent(p):
        remote(arrived1.at[p], arrived1.at[p], s1.at[p], rn.at[0], mate).wait_send()
        remote(others(summed, p), others(arrived2, p), s2.at[p], r2.at[p], mate).wait_send()
        all_totals(p).wait_send()

    def sent_copies(p):
        for i, d, ok in own_ways():
            pl.when(ok)(whole(a, p, so.at[i, p]).wait_send)
        for d in range(2, outer - 1):
            for far in (d, -d):
                ok, sem, _ = relays(far)
                z = a - far
                there = z >= 0 if far > 0 else z <= outer - 1
                pl.when(jnp.logical_and(ok, there))(whole(z, p, sem.at[p]).wait_send)
        crossed(p, outer - p).wait_send()

    onward(0, 0)
    hear(1, outer)
    for k in range(1, chunks):
        onward(k, 0)
    gather(0)
    for k in order_of[1]:
        onward(k, 1)
    def play(plan, inward, at_end):
        later = []
        away = {"near": 1, "mid": 2, "end": 3} if at_end else {"near": -1, "inner": 1, "far": 2}
        reach = dict(away, far=2)
        for i, (kind, *rest) in enumerate(plan):
            if kind in ("pass", "beside") or i == len(plan) - 1:
                while later:
                    later.pop()()
            if i == len(plan) - 3:
                sent(0)
                sent(1)
            if kind == "gather":
                gather(1)
            elif kind == "finish":
                later.append(scaled(rest[0]))
            elif kind == "beside":
                own_across(1 - b, rest[0]).wait_recv()
                beside(a, rest[0]).start()
            elif rest[0] == "mate":
                _, p, h = rest
                (own_across(b, h) if p else across(a, b, p, h)).start()
            elif kind == "own":
                way, p, h = rest
                line_copy(a, p, h, so.at[0, p], a + inward * reach[way]).start()
            else:
                way, p, h = rest
                z = a + inward * away[way]
                line_copy(z, p, h, sn.at[0], a).wait_recv()
                if not at_end and (way == "far" or way == "inner" and MIDDLE_RELAYS[p]):
                    line_copy(z, p, h, so.at[0, p], a - inward).start()
                if p == 0 or way != "near":
                    across(z, b, p, h).start()

    def z_sent(p):
        for blocks, here in ((2, at_end), (4, jnp.logical_not(at_end))):
            ref = copy.at[p, pl.ds(0, blocks * rows)]
            pl.when(here)(remote(ref, ref, so.at[0, p], rn.at[0], mate).wait_send)

    if planned:
        inward = jnp.where(a < outer // 2, 1, -1)
        at_end = jnp.logical_or(a == 0, a == outer - 1)
        pl.when(at_end)(lambda: play(END_PLAN, inward, True))
        pl.when(jnp.logical_not(at_end))(lambda: play(MIDDLE_PLAN, inward, False))
        z_sent(0)
        crossed(0, outer).wait_send()
        crossed(0, outer).wait_recv()
        crossed(1, outer - 2).wait_recv()
        z_sent(1)
        crossed(1, outer - 1).wait_send()
    else:
        gather(1)
        finish(0)

        def due(d, p, h):
            return 4.7 * p + (4.5 + 1.4 * h if d == 1 else 5.2 + 4 * (d - 2) + 3.8 * h)

        def pass_on(h):
            own_across(1 - b, h).wait_recv()
            beside(a, h).start()

        todo = [(4.6, lambda: finish(1)), (9, lambda: sent(0)), (9, lambda: sent(1))]
        for h in range(cut):
            for d in range(1, outer):
                for p in range(2):
                    todo.append((due(d, p, h), functools.partial(forward, d, p, h)))
            todo.append((due(2, 1, h) + 0.1, functools.partial(pass_on, h)))
        todo.append((due(outer - 1, 1, cut - 1) - 0.1, lambda: sent_copies(0)))
        for _, act in sorted(todo, key=lambda item: item[0]):
            act()
        crossed(0, outer).wait_recv()
        if outer > 2:
            crossed(1, outer - 2).wait_recv()
        sent_copies(1)
    whole_beside().wait_recv()
    whole_beside().wait_send()


def store(step, new, copy, mom, sqr, *rest):
    outs, sem = rest[:10], rest[10]
    srcs = [ref.at[p] for ref in (step, new, copy, mom, sqr) for p in range(2)]
    order = (4, 5, 0, 1, 2, 3, 6, 7, 8, 9)
    moves = [pltpu.make_async_copy(srcs[i], outs[i], sem.at[i]) for i in order]
    for move in moves:
        move.start()
    for move in moves:
        move.wait()


def per_device(n, t, x, cq, cv, wq, wv, bq, bv, fq, sq, fv, sv):
    tokens, depth = x.shape
    rows, cols = wq.shape
    wide = fq.shape[1]
    outer = n // 2
    chunks = depth // max(2 * rows, min(depth, 256))
    cut = CUT if rows % (16 * CUT) == 0 else 1
    planned = outer == 4 and cut == CUT
    fine = cut
    hbm = pl.BlockSpec(memory_space=pltpu.HBM)
    vmem = pl.BlockSpec(memory_space=pltpu.VMEM)
    shape = jax.ShapeDtypeStruct
    dma = pltpu.SemaphoreType.DMA
    kept = (
        pltpu.VMEM((2, rows, cols), F32),
        pltpu.VMEM((2, rows, cols), F32),
        pltpu.VMEM((2, depth, cols), BF16),
        pltpu.VMEM((2, rows, wide), F32),
        pltpu.VMEM((2, rows, wide), F32),
    )
    held = pl.pallas_call(
        functools.partial(body, n, t),
        out_shape=kept,
        in_specs=[hbm] * 11,
        out_specs=[vmem] * 5,
        scratch_shapes=[
            pltpu.VMEM((tokens, depth), BF16),
            pltpu.VMEM((2, tokens, cols), BF16),
            pltpu.VMEM((2, rows, cols), F32),
            pltpu.VMEM((2, RK, cols), BF16),
            pltpu.VMEM((2, rows, wide), F32),
            pltpu.VMEM((2, rows, wide), F32),
            pltpu.VMEM((tokens, 2 * wide), BF16),
            pltpu.VMEM((2, depth, wide), BF16),
            pltpu.VMEM((2, outer, rows, wide), BF16),
            pltpu.VMEM((2, outer, rows, wide), BF16),
            pltpu.VMEM((2, outer, rows, wide), BF16),
            pltpu.VMEM((2, rows, cols), F32),
            pltpu.VMEM((2, 1, 1, wide), F32),
            pltpu.VMEM((2, n * t, 1, wide), F32),
            dma((5,)),
            dma((chunks,)),
            dma((2,)),
            dma((outer, 2, fine)),
            dma((2,)),
            dma((2,)),
            dma((2,)),
            dma((2,)),
            dma((1 if planned else 4, 2)),
            dma((1, 1, 1) if planned else (2, max(outer - 3, 1), 2)),
            dma((2,)),
            dma((2,)),
            dma((1,)),
            dma((1,)),
            dma((cut,)),
            pltpu.SemaphoreType.REGULAR((2,)),
        ],
        compiler_params=pltpu.CompilerParams(
            collective_id=0, has_side_effects=True, vmem_limit_bytes=62 * 10**6
        ),
        name="update",
    )(x, cq, cv, wq, wv, bq.T, bv.T, fq, sq, fv, sv)
    full, half = shape((rows, cols), F32), shape((rows, wide), F32)
    whole = shape((depth, cols), BF16)
    outs = pl.pallas_call(
        store,
        out_shape=(full,) * 4 + (whole,) * 2 + (half,) * 4,
        in_specs=[vmem] * 5,
        out_specs=[hbm] * 10,
        scratch_shapes=[dma((10,))],
        compiler_params=pltpu.CompilerParams(vmem_limit_bytes=40 * 2**20),
        name="store",
    )(*held)
    return tuple(outs[i] for i in (0, 1, 2, 3, 4, 5, 6, 8, 7, 9))


def solution(mesh):
    split = P("fs", "tp")
    return jax.shard_map(
        functools.partial(per_device, mesh.shape["fs"], mesh.shape["tp"]),
        mesh=mesh,
        in_specs=(P("fs", None),) + (split,) * 4 + (P("tp", None),) * 2 + (split,) * 4,
        out_specs=(split,) * 4 + (P(None, "tp"),) * 2 + (split,) * 4,
        check_vma=False,
    )
```

```python
import functools

import jax
import jax.numpy as jnp
from jax import lax
from jax.experimental import pallas as pl
from jax.experimental.pallas import tpu as pltpu
from jax.sharding import PartitionSpec as P

HEAD = 64
RK = 32
CUT = 2
MESH = pl.DeviceIdType.MESH
END_PLAN = (
    ("finish", 0), ("own", "near", 0, 0), ("own", "mate", 0, 1), ("gather", 1),
    ("own", "mate", 0, 0), ("own", "near", 0, 1), ("pass", "near", 0, 1), ("own", "far", 0, 1),
    ("pass", "near", 0, 0), ("own", "far", 0, 0), ("pass", "mid", 0, 0), ("finish", 1),
    ("own", "mate", 1, 0), ("own", "mate", 1, 1), ("own", "far", 1, 1), ("own", "far", 1, 0),
    ("pass", "mid", 0, 1), ("own", "near", 1, 1), ("pass", "end", 0, 1), ("pass", "mid", 1, 1),
    ("pass", "end", 0, 0), ("pass", "mid", 1, 0), ("own", "near", 1, 0), ("pass", "near", 1, 0),
    ("pass", "end", 1, 1), ("beside", 1), ("beside", 0), ("pass", "end", 1, 0),
    ("pass", "near", 1, 1),
)
MIDDLE_PLAN = (
    ("finish", 0), ("own", "inner", 0, 0), ("own", "near", 0, 1), ("own", "mate", 0, 1),
    ("own", "inner", 0, 1), ("own", "mate", 0, 0), ("own", "near", 0, 0), ("gather", 1),
    ("pass", "inner", 0, 0), ("pass", "inner", 0, 1), ("pass", "near", 0, 1),
    ("pass", "near", 0, 0), ("finish", 1), ("own", "far", 1, 1), ("pass", "far", 0, 1),
    ("pass", "far", 0, 0), ("own", "near", 1, 0), ("own", "mate", 1, 0), ("pass", "far", 1, 1),
    ("own", "far", 1, 0), ("own", "mate", 1, 1), ("pass", "far", 1, 0), ("own", "inner", 1, 0),
    ("pass", "near", 1, 1), ("own", "inner", 1, 1), ("own", "near", 1, 1), ("beside", 0),
    ("pass", "inner", 1, 0), ("pass", "inner", 1, 1), ("beside", 1), ("pass", "near", 1, 0),
)
MIDDLE_RELAYS = (True, False)
F32 = jnp.float32
BF16 = jnp.bfloat16


def flip(x, bits):
    out, weight = x, 1
    while weight <= bits:
        if bits & weight:
            out = out + weight * (1 - 2 * ((x // weight) % 2))
        weight *= 2
    return out


def remote(src, dst, send, recv, to):
    return pltpu.make_async_remote_copy(
        src_ref=src, dst_ref=dst, send_sem=send, recv_sem=recv, device_id=to, device_id_type=MESH
    )


def body(
    n,
    t,
    x_hbm,
    cq_hbm,
    cv_hbm,
    wq_hbm,
    wv_hbm,
    bq_hbm,
    bv_hbm,
    fq_hbm,
    sq_hbm,
    fv_hbm,
    sv_hbm,
    step,
    new,
    copy,
    mom,
    sqr,
    x,
    cot,
    w,
    basis,
    first,
    second,
    small,
    part,
    summed,
    arrived1,
    arrived2,
    raw,
    tot,
    tot_all,
    in_sem,
    x_sem,
    s1,
    r1,
    s2,
    r2,
    st,
    rt,
    so,
    sr,
    sy,
    ry,
    sn,
    rn,
    rm,
    line,
):
    f = lax.axis_index("fs")
    g = lax.axis_index("tp")
    me = f * t + g
    count = n * t
    outer = n // 2
    a, b = f // 2, f % 2
    mate = (a * 2 + 1 - b, g)
    depth = x.shape[1]
    rows = depth // n
    cols = w.shape[2]
    wide = cols // HEAD * RK
    cut = r1.shape[2]
    rz = r1
    planned = outer == 4 and cut == CUT
    bit = rows // cut
    fine = r1.shape[2]
    slip = rows // fine

    chunk = max(2 * rows, min(depth, 256))
    chunks = depth // chunk
    pairs = chunk // (2 * rows)
    order = list(range(chunks // 2, chunks)) + list(range(chunks // 2 - 1, -1, -1))
    at = a // pairs

    def chunk_at(k):
        return pl.ds(pl.multiple_of(flip(at, order[k]) * chunk, chunk), chunk)

    sources = ((bq_hbm, bv_hbm), (cq_hbm, cv_hbm), (fq_hbm, fv_hbm), (sq_hbm, sv_hbm), (wq_hbm, wv_hbm))
    holders = (basis, cot, first, second, w)

    def load(i):
        for p in range(2):
            pltpu.make_async_copy(sources[i][p], holders[i].at[p], in_sem.at[i]).start()

    def loaded(i):
        pltpu.make_async_copy(holders[i], holders[i], in_sem.at[i]).wait()

    x_loads = [
        pltpu.make_async_copy(x_hbm.at[:, chunk_at(k)], x.at[:, chunk_at(k)], x_sem.at[k])
        for k in range(chunks)
    ]
    load(0)
    load(1)
    x_loads[0].start()

    barrier = pltpu.get_barrier_semaphore()

    def hello(to):
        pl.semaphore_signal(barrier, inc=1, device_id=to, device_id_type=MESH)

    def at_line(z):
        return (z * 2 + b, g)

    def greet_line(i, c):
        hello(at_line((a + 1 + i) % outer))
        return c

    chained = outer <= 8
    below, above = a > 0, a < outer - 1
    hello(mate)
    if chained:
        pl.when(below)(lambda: hello(at_line(a - 1)))
        pl.when(above)(lambda: hello(at_line(a + 1)))
        near_by = below.astype(jnp.int32) + above.astype(jnp.int32)
    else:
        lax.fori_loop(0, outer - 1, greet_line, 0)
        near_by = outer - 1
    for i in range(1, t):
        hello((f, (g + i) % t))

    def tell(way, z):
        pl.semaphore_signal(
            line.at[way], inc=1, device_id=at_line(z), device_id_type=MESH
        )

    def tell_neighbours():
        if chained:

            @pl.when(jnp.logical_and(below, above))
            def _():
                tell(0, a - 1)
                tell(1, a + 1)

    def hear(start, stop):
        if chained:
            for way, number, go, to in (
                (0, outer - 2 - a, below, a - 1),
                (1, a - 1, above, a + 1),
            ):

                def pass_along(i, c, way=way, go=go, to=to):
                    pl.semaphore_wait(line.at[way], 1)
                    pl.when(go)(lambda: tell(way, to))
                    return c

                lax.fori_loop(start, jnp.clip(number, start, stop), pass_along, 0)

    for x_load in x_loads[1:]:
        x_load.start()
    for i in range(2, 5):
        load(i)
    loaded(0)

    spread = (
        lax.broadcasted_iota(jnp.int32, (RK, wide), 1) % RK
        == lax.broadcasted_iota(jnp.int32, (RK, wide), 0)
    ).astype(BF16)
    own_head = (
        lax.broadcasted_iota(jnp.int32, (cols, wide), 0) // HEAD
        == lax.broadcasted_iota(jnp.int32, (cols, wide), 1) // RK
    )
    diag = [
        jnp.where(
            own_head,
            lax.dot_general(basis[p], spread, (((0,), (0,)), ((), ())), preferred_element_type=F32),
            0.0,
        ).astype(BF16)
        for p in range(2)
    ]
    loaded(1)
    for p in range(2):
        small[:, p * wide : (p + 1) * wide] = jnp.dot(
            cot[p], diag[p], preferred_element_type=F32
        ).astype(BF16)

    def block(z, half):
        return pl.ds(pl.multiple_of((z * 2 + half) * rows, rows), rows)

    def first_copy(k, i, p, h):
        z = flip(at, order[k]) * pairs + i
        there = pl.ds(h * slip, slip)
        return remote(
            part.at[p, pl.ds(pl.multiple_of((z * 2 + 1 - b) * rows + h * slip, slip), slip)],
            arrived1.at[p, z, there],
            s1.at[p],
            r1.at[k * pairs + i, p, h],
            mate,
        )

    def first_starts(k, p):
        for i in range(pairs):
            for h in range(fine):
                first_copy(k, i, p, h).start()

    def multiply(here):
        sums = lax.dot_general(
            x[:, here], small[...], (((0,), (0,)), ((), ())), preferred_element_type=F32
        ).astype(BF16)
        for p in range(2):
            part[p, here] = sums[:, p * wide : (p + 1) * wide]

    apart = rows % 128 == 0
    order_of = (list(range(chunks)), list(range(chunks)))
    if chunks == 4:
        order_of = (order_of[0], [0, 2, 1, 3])
    for k in range(chunks):
        x_loads[k].wait()
        multiply(block(flip(at, order[k]), 1 - b) if apart else chunk_at(k))
        if k == 0:
            pl.semaphore_wait(barrier, near_by + t)
        first_starts(k, 0)
        if k == 0:
            tell_neighbours()
    for k in order_of[1]:
        first_starts(k, 1)
    hear(0, 1)
    if apart:
        for k in range(chunks):
            multiply(block(flip(at, order[k]), b))

    def onward(k, p):
        for i in range(pairs):
            z = flip(at, order[k]) * pairs + i
            for h in range(fine):
                first_copy(k, i, p, h).wait_recv()
                if k < chunks - 1 or pairs > 1:
                    there = pl.ds(h * slip, slip)
                    send = remote(
                        summed.at[p, z, there],
                        arrived2.at[p, a, there],
                        s2.at[p],
                        r2.at[p],
                        (z * 2 + b, g),
                    )
                    mine = pl.ds(pl.multiple_of((z * 2 + b) * rows + h * slip, slip), slip)
                    summed[p, z, there] = (
                        part[p, mine].astype(F32) + arrived1[p, z, there].astype(F32)
                    ).astype(BF16)
                    if k < chunks - 1:
                        send.start()
                    else:
                        pl.when(z != a)(send.start)

    def others(ref, p):
        return ref.at[p, pl.ds(0, outer - 1)]

    back = (((1,), (1,)), ((), ()))

    def gather(p):
        reduced = part[p, block(a, b)].astype(F32) + arrived1[p, a].astype(F32)
        remote(others(summed, p), others(arrived2, p), s2.at[p], r2.at[p], mate).wait_recv()
        for q in range(outer - 1, 0, -1):
            reduced = reduced + arrived2[p, flip(a, q)].astype(F32)
        if p == 0:
            for i in range(2, 5):
                loaded(i)
        moment = 0.9 * first[p] + 0.1 * reduced
        square = 0.95 * second[p] + 0.05 * reduced * reduced
        direction = moment / (jnp.sqrt(square) + 1e-08)
        tot[p, 0] = jnp.sum(direction * direction, axis=0, keepdims=True)

        def send_total(to):
            remote(tot.at[p, 0], tot_all.at[p, me], st.at[p], rt.at[p], to).start()

        def send_row(i, c):
            to = f + n // 2 + i
            to = to - n * (to // n)
            for h in range(t):
                send_total((to, h))
            return c

        lax.fori_loop(0, n // 2, send_row, 0)
        lax.fori_loop(n // 2 + 1, n, send_row, 0)
        for i in range(1, t):
            send_total((f, (g + i) % t))
        tot_all[p, me] = tot[p, 0]
        mom[p] = moment
        sqr[p] = square
        upper = direction.astype(BF16)
        lower = (direction - upper.astype(F32)).astype(BF16)
        raw[p] = lax.dot_general(upper, diag[p], back, preferred_element_type=F32) + lax.dot_general(
            lower, diag[p], back, preferred_element_type=F32
        )

    entries = depth * wide * t

    def all_totals(p):
        ref = tot_all.at[p, pl.ds(0, count - 1)]
        return remote(ref, ref, st.at[p], rt.at[p], mate)

    def piece(z, half, p, h):
        return copy.at[p, pl.ds(pl.multiple_of((z * 2 + half) * rows + h * bit, bit), bit)]

    def line_copy(z, p, h, sem, to):
        ref = piece(z, b, p, h)
        return remote(ref, ref, sem, rz.at[z, p, h], (to * 2 + b, g))

    def across(z, half, p, h):
        ref = piece(z, half, p, h)
        return remote(ref, ref, sy.at[p], ry.at[p], mate)

    def own_across(half, h):
        ref = piece(a, half, 1, h)
        return remote(ref, ref, sy.at[1], rm.at[h], mate)

    def crossed(p, blocks):
        ref = copy.at[p, pl.ds(0, blocks * rows)]
        return remote(ref, ref, sy.at[p], ry.at[p], mate)

    near = flip(a, 1)

    def beside(z, h):
        ref = piece(z, 1 - b, 1, h)
        return remote(ref, ref, sn.at[0], rn.at[0], (near * 2 + b, g))

    def whole_beside():
        ref = copy.at[1, block(a, b)]
        return remote(ref, ref, sn.at[0], rn.at[0], mate)

    def own_ways():
        for i, d in enumerate((2, -2, 1, -1)):
            yield i, d, a + d <= outer - 1 if d > 0 else a + d >= 0

    def scaled(p):
        all_totals(p).wait_recv()
        mean = jnp.sum(jnp.sum(tot_all[p], axis=0), axis=1, keepdims=True) / entries
        scale = 1.0 / jnp.sqrt(mean + 0.25)
        move = scale * raw[p]
        fresh = w[p] - 0.1 * move
        copy[p, block(a, b)] = fresh.astype(BF16)

        def keep():
            step[p] = move
            new[p] = fresh

        return keep

    def finish(p):
        keep = scaled(p)
        for h in range(cut):
            for i, d, ok in own_ways():
                pl.when(ok)(line_copy(a, p, h, so.at[i, p], a + d).start)
            (own_across(b, h) if p else across(a, b, p, h)).start()
        keep()

    def whole(z, p, sem):
        ref = copy.at[p, block(z, b)]
        return remote(ref, ref, sem, rn.at[0], mate)

    def relays(far):
        up = far > 0
        return (a < outer - 1 if up else a > 0), (sr.at[int(up), abs(far) - 2]), a + (1 if up else -1)

    def forward(d, p, h):
        for far in (d, -d):
            z = a - far

            def handle(far=far, z=z):
                line_copy(z, p, h, sn.at[0], a).wait_recv()
                if 2 <= d < outer - 1:
                    ok, sem, to = relays(far)
                    pl.when(ok)(line_copy(z, p, h, sem.at[p], to).start)
                if d == 1 and p == 1:
                    pl.when(z != near)(lambda: across(z, b, p, h).start())
                else:
                    across(z, b, p, h).start()

            pl.when(z >= 0 if far > 0 else z <= outer - 1)(handle)

    def sent(p):
        remote(arrived1.at[p], arrived1.at[p], s1.at[p], rn.at[0], mate).wait_send()
        remote(others(summed, p), others(arrived2, p), s2.at[p], r2.at[p], mate).wait_send()
        all_totals(p).wait_send()

    def sent_copies(p):
        for i, d, ok in own_ways():
            pl.when(ok)(whole(a, p, so.at[i, p]).wait_send)
        for d in range(2, outer - 1):
            for far in (d, -d):
                ok, sem, _ = relays(far)
                z = a - far
                there = z >= 0 if far > 0 else z <= outer - 1
                pl.when(jnp.logical_and(ok, there))(whole(z, p, sem.at[p]).wait_send)
        crossed(p, outer - p).wait_send()

    onward(0, 0)
    hear(1, outer)
    for k in range(1, chunks):
        onward(k, 0)
    gather(0)
    for k in order_of[1]:
        onward(k, 1)
    def play(plan, inward, at_end):
        later = []
        away = {"near": 1, "mid": 2, "end": 3} if at_end else {"near": -1, "inner": 1, "far": 2}
        reach = dict(away, far=2)
        for i, (kind, *rest) in enumerate(plan):
            if kind in ("pass", "beside") or i == len(plan) - 1:
                while later:
                    later.pop()()
            if i == len(plan) - 3:
                sent(0)
                sent(1)
            if kind == "gather":
                gather(1)
            elif kind == "finish":
                later.append(scaled(rest[0]))
            elif kind == "beside":
                own_across(1 - b, rest[0]).wait_recv()
                beside(a, rest[0]).start()
            elif rest[0] == "mate":
                _, p, h = rest
                (own_across(b, h) if p else across(a, b, p, h)).start()
            elif kind == "own":
                way, p, h = rest
                line_copy(a, p, h, so.at[0, p], a + inward * reach[way]).start()
            else:
                way, p, h = rest
                z = a + inward * away[way]
                line_copy(z, p, h, sn.at[0], a).wait_recv()
                if not at_end and (way == "far" or way == "inner" and MIDDLE_RELAYS[p]):
                    line_copy(z, p, h, so.at[0, p], a - inward).start()
                if p == 0 or way != "near":
                    across(z, b, p, h).start()

    def z_sent(p):
        for blocks, here in ((2, at_end), (4, jnp.logical_not(at_end))):
            ref = copy.at[p, pl.ds(0, blocks * rows)]
            pl.when(here)(remote(ref, ref, so.at[0, p], rn.at[0], mate).wait_send)

    if planned:
        inward = jnp.where(a < outer // 2, 1, -1)
        at_end = jnp.logical_or(a == 0, a == outer - 1)
        pl.when(at_end)(lambda: play(END_PLAN, inward, True))
        pl.when(jnp.logical_not(at_end))(lambda: play(MIDDLE_PLAN, inward, False))
        z_sent(0)
        crossed(0, outer).wait_send()
        crossed(0, outer).wait_recv()
        crossed(1, outer - 2).wait_recv()
        z_sent(1)
        crossed(1, outer - 1).wait_send()
    else:
        gather(1)
        finish(0)

        def due(d, p, h):
            return 4.7 * p + (4.5 + 1.4 * h if d == 1 else 5.2 + 4 * (d - 2) + 3.8 * h)

        def pass_on(h):
            own_across(1 - b, h).wait_recv()
            beside(a, h).start()

        todo = [(4.6, lambda: finish(1)), (9, lambda: sent(0)), (9, lambda: sent(1))]
        for h in range(cut):
            for d in range(1, outer):
                for p in range(2):
                    todo.append((due(d, p, h), functools.partial(forward, d, p, h)))
            todo.append((due(2, 1, h) + 0.1, functools.partial(pass_on, h)))
        todo.append((due(outer - 1, 1, cut - 1) - 0.1, lambda: sent_copies(0)))
        for _, act in sorted(todo, key=lambda item: item[0]):
            act()
        crossed(0, outer).wait_recv()
        if outer > 2:
            crossed(1, outer - 2).wait_recv()
        sent_copies(1)
    whole_beside().wait_recv()
    whole_beside().wait_send()


def store(step, new, copy, mom, sqr, *rest):
    outs, sem = rest[:10], rest[10]
    srcs = [ref.at[p] for ref in (step, new, copy, mom, sqr) for p in range(2)]
    order = (4, 5, 0, 1, 2, 3, 6, 7, 8, 9)
    moves = [pltpu.make_async_copy(srcs[i], outs[i], sem.at[i]) for i in order]
    for move in moves:
        move.start()
    for move in moves:
        move.wait()


def per_device(n, t, x, cq, cv, wq, wv, bq, bv, fq, sq, fv, sv):
    tokens, depth = x.shape
    rows, cols = wq.shape
    wide = fq.shape[1]
    outer = n // 2
    chunks = depth // max(2 * rows, min(depth, 256))
    cut = CUT if rows % (16 * CUT) == 0 else 1
    planned = outer == 4 and cut == CUT
    fine = cut
    hbm = pl.BlockSpec(memory_space=pltpu.HBM)
    vmem = pl.BlockSpec(memory_space=pltpu.VMEM)
    shape = jax.ShapeDtypeStruct
    dma = pltpu.SemaphoreType.DMA
    kept = (
        pltpu.VMEM((2, rows, cols), F32),
        pltpu.VMEM((2, rows, cols), F32),
        pltpu.VMEM((2, depth, cols), BF16),
        pltpu.VMEM((2, rows, wide), F32),
        pltpu.VMEM((2, rows, wide), F32),
    )
    held = pl.pallas_call(
        functools.partial(body, n, t),
        out_shape=kept,
        in_specs=[hbm] * 11,
        out_specs=[vmem] * 5,
        scratch_shapes=[
            pltpu.VMEM((tokens, depth), BF16),
            pltpu.VMEM((2, tokens, cols), BF16),
            pltpu.VMEM((2, rows, cols), F32),
            pltpu.VMEM((2, RK, cols), BF16),
            pltpu.VMEM((2, rows, wide), F32),
            pltpu.VMEM((2, rows, wide), F32),
            pltpu.VMEM((tokens, 2 * wide), BF16),
            pltpu.VMEM((2, depth, wide), BF16),
            pltpu.VMEM((2, outer, rows, wide), BF16),
            pltpu.VMEM((2, outer, rows, wide), BF16),
            pltpu.VMEM((2, outer, rows, wide), BF16),
            pltpu.VMEM((2, rows, cols), F32),
            pltpu.VMEM((2, 1, 1, wide), F32),
            pltpu.VMEM((2, n * t, 1, wide), F32),
            dma((5,)),
            dma((chunks,)),
            dma((2,)),
            dma((outer, 2, fine)),
            dma((2,)),
            dma((2,)),
            dma((2,)),
            dma((2,)),
            dma((1 if planned else 4, 2)),
            dma((1, 1, 1) if planned else (2, max(outer - 3, 1), 2)),
            dma((2,)),
            dma((2,)),
            dma((1,)),
            dma((1,)),
            dma((cut,)),
            pltpu.SemaphoreType.REGULAR((2,)),
        ],
        compiler_params=pltpu.CompilerParams(
            collective_id=0, has_side_effects=True, vmem_limit_bytes=62 * 10**6
        ),
        name="update",
    )(x, cq, cv, wq, wv, bq.T, bv.T, fq, sq, fv, sv)
    full, half = shape((rows, cols), F32), shape((rows, wide), F32)
    whole = shape((depth, cols), BF16)
    outs = pl.pallas_call(
        store,
        out_shape=(full,) * 4 + (whole,) * 2 + (half,) * 4,
        in_specs=[vmem] * 5,
        out_specs=[hbm] * 10,
        scratch_shapes=[dma((10,))],
        compiler_params=pltpu.CompilerParams(vmem_limit_bytes=40 * 2**20),
        name="store",
    )(*held)
    return tuple(outs[i] for i in (0, 1, 2, 3, 4, 5, 6, 8, 7, 9))


def solution(mesh):
    split = P("fs", "tp")
    return jax.shard_map(
        functools.partial(per_device, mesh.shape["fs"], mesh.shape["tp"]),
        mesh=mesh,
        in_specs=(P("fs", None),) + (split,) * 4 + (P("tp", None),) * 2 + (split,) * 4,
        out_specs=(split,) * 4 + (P(None, "tp"),) * 2 + (split,) * 4,
        check_vma=False,
    )
```
